32 devices in a mesh: sp: 8 (over z, y), tp: 4 (over x, core).
Axes of the slice: x: 2, y: 2, z: 4, core: 2. Of those that a mesh axis runs over, the one named last changes fastest.
Arguments:
- hidden: bfloat16 [2048, 2048], P('sp'), may hold values from -6 to 6
- cotangent: bfloat16 [2048, 2048], P('sp'), may hold values from -6 to 6
- retained: bfloat16 [2048, 2048], P('sp', 'tp'), may hold values from -6 to 6
- queries: bfloat16 [2048, 1024], P('sp', 'tp'), may hold values from -1.5 to 1.5
- key_rows: bfloat16 [2048, 1024], P('sp', 'tp'), may hold values from -1.5 to 1.5
- value_rows: bfloat16 [2048, 2048], P('sp', 'tp'), may hold values from -0.25 to 0.25
- routes: int32 [2048, 2], P('sp'), may hold values from 0 to 7, all different within a row; in each aligned block of 256 rows (0 to 255, 256 to 511, ...) at most 96 rows name the same one
- route_weight: float32 [2048, 2], P('sp'), may hold values from 0.2 to 1.5
- gate_weight: bfloat16 [8, 2048, 1024], P('sp', None, 'tp'), may hold values from -0.125 to 0.125
- up_weight: bfloat16 [8, 2048, 1024], P('sp', None, 'tp'), may hold values from -0.125 to 0.125
- down_weight: bfloat16 [8, 1024, 2048], P('sp', 'tp'), may hold values from -0.1875 to 0.1875
- out_weight: bfloat16 [2048, 2048], P(None, 'tp'), may hold values from -0.125 to 0.125
Outputs:
- gate_grad: float32 [8, 2048, 1024], P('sp', None, 'tp')
- up_grad: float32 [8, 2048, 1024], P('sp', None, 'tp')
- down_grad: float32 [8, 1024, 2048], P('sp', 'tp')
- proj_grad: float32 [2048, 2048], P('sp', 'tp')
- query_gradient: float32 [2048, 1024], P('sp', 'tp')
- key_gradient: float32 [2048, 1024], P('sp', 'tp')
- value_gradient: float32 [2048, 2048], P('sp', 'tp')
The draws below stay inside these ranges and needn't reach their ends.
Inputs may be any that keep to these rules, and one draw needn't show every extreme that they name: `routes`: each row names 2 different experts; among the 256 rows of one index of sp no expert is named more than 96 times, a bound that some block reaches.
All inputs are finite; a program needn't handle non-finite values.
Results may differ from the reference program's by a relative error of at most 0.013.
Values may be sent and summed in bfloat16 or wider, within the bound.
No kernel may reach another device: no remote copies, remote signals or barrier semaphores. Data moves between devices by JAX's collectives and lax.ppermute only.
A program may use at most 128 MiB of HBM per device.

```python
import math
import jax
import jax.numpy as jnp
import numpy as np
from jax import lax

D = 2048
H = 4
DK = 256
DV = 512
FF = 1024
TOP = 2
TOK_DEV = 256
TOKENS = 2048
EXPERTS = 8
CAP = 96
VW = 2048
N_SP = 8
N_TP = 4


def with_spikes(array, own_key, source, target, blocks, factor):
    owner, partner = [(jnp.arange(array.shape[position]) // (array.shape[position] // blocks)).reshape([-1 if axis == position else 1 for axis in range(array.ndim)]) for position in (source, target)]
    chosen = jax.random.permutation(own_key, blocks)[partner]
    strong = (owner == chosen) | (owner == (partner + blocks // 2) % blocks)
    return jnp.where(strong, factor * array, array)


def block_scale(own_key, shape, cuts, smallest, largest):
    level = 1.0
    for position, blocks in cuts:
        heights = jax.random.uniform(jax.random.fold_in(jax.random.fold_in(own_key, 6), position), (blocks,), jnp.float32, smallest / len(cuts), largest / len(cuts))
        level = level * jnp.repeat(jnp.exp(heights), shape[position] // blocks).reshape((-1,) + (1,) * (len(shape) - 1 - position))
    return level


def assign_block(key, own, number, rows, number_of, top, most, skew):
    sequence = jax.random.permutation(key, number_of)
    heavy_load, ordinary = portions_of(number_of, rows * top, most, skew, True), portions_of(number_of, rows * top, most, skew, False)
    places = jnp.arange(number_of)

    def named(tallies, offset_by):
        used = int((tallies > 0).sum())
        fixed = max(1, used // 4)
        passed = fixed + (places - fixed + offset_by * (used - fixed)) % max(1, number_of - fixed)
        return jnp.zeros((number_of,), jnp.int32).at[sequence[jnp.where(places < fixed, places, passed)]].set(jnp.asarray(tallies, jnp.int32))

    tallies = jnp.where(number % 4 == 0, named(heavy_load, number // 4), named(ordinary, number - number // 4 - 1))
    mixed = jax.random.permutation(jax.random.fold_in(own, 3), number_of)
    source_of, receiver = mixed[0:number_of // 2 * 2:2], mixed[1:number_of // 2 * 2:2]
    slack = jnp.minimum(tallies[source_of] - 1, most - tallies[receiver]) // 2
    slack = jnp.where((source_of == sequence[0]) | (receiver == sequence[0]) | (tallies[receiver] == 0), 0, jnp.maximum(slack, 0))
    passed = jax.random.randint(jax.random.fold_in(own, 4), (number_of // 2,), 0, 1 << 20) % (slack + 1)
    tallies = tallies.at[source_of].add(-passed).at[receiver].add(passed)
    members = jnp.searchsorted(jnp.cumsum(tallies), jnp.arange(rows * top), side="right").astype(jnp.int32)
    listing = members.reshape(top, rows).T
    listing = listing[jax.random.permutation(jax.random.fold_in(own, 1), rows)]
    offset_by = jax.random.randint(jax.random.fold_in(own, 2), (rows, 1), 0, top)
    return jnp.take_along_axis(listing, (jnp.arange(top)[None, :] + offset_by) % top, axis=1)


def portions_of(number_of, total, reach, lean, full):
    weights = [(1 << 20) // math.isqrt(rank ** lean) + 1 for rank in range(1, number_of + 1)]
    largest = reach if full else min(reach, max(-(-total // number_of), total * weights[0] // sum(weights)))
    least = 1 if total - largest >= number_of - 1 else 0
    counts, surplus = [largest] + [least] * (number_of - 1), total - largest - least * (number_of - 1)
    while surplus > 0:
        movable = [i for i in range(1, number_of) if counts[i] < largest] or [i for i in range(1, number_of) if counts[i] < reach]
        mass, left = sum([weights[i] for i in movable]), surplus
        for i in movable:
            addition = min(reach - counts[i], max(1, left * weights[i] // mass), surplus)
            counts[i] = counts[i] + addition
            surplus = surplus - addition
    return np.array(counts)


def centred(rng, dims, scale, limit, cuts=(), kind=jnp.bfloat16):
    entries = scale * jax.random.normal(rng, dims, jnp.float32)
    if cuts:
        entries = entries * block_scale(rng, dims, cuts, -0.22, 0.18)
    return jnp.clip(entries, -limit, limit).astype(kind)


def bell_draw_with(key, dims, width, limit, cuts, heavy, kind=jnp.bfloat16):
    entries = width * jax.random.normal(key, dims, jnp.float32)
    if cuts:
        entries = entries * block_scale(key, dims, cuts, -0.22, 0.18)
    return jnp.clip(with_spikes(entries, jax.random.fold_in(key, 3), *heavy), -limit, limit).astype(kind)


def setup_inputs(seed: int = 0) -> dict:
    keys = jax.random.split(jax.random.key(seed), 13)
    hidden = centred(keys[0], (TOKENS, D), 1.0, 6.0, ((0, 8),))
    cotangent = bell_draw_with(keys[1], (TOKENS, D), 1.0, 6.0, ((0, 8),), (0, 1, 8, 2.0))
    retained = centred(keys[2], (TOKENS, VW), 1.0, 6.0, ((0, 8), (1, 4)))
    queries = centred(keys[3], (TOKENS, H * DK), 0.25, 1.5, ((0, 8), (1, 4)))
    key_rows = centred(keys[4], (TOKENS, H * DK), 0.25, 1.5, ((0, 8), (1, 4)))
    value_rows = centred(keys[5], (TOKENS, VW), DV ** -0.5, 0.25, ((0, 8), (1, 4)))
    routes_keys = jax.random.split(jax.random.fold_in(keys[6], 1), TOKENS // TOK_DEV)
    routes_turns = jax.random.permutation(jax.random.fold_in(keys[6], 3), TOKENS // TOK_DEV)
    routes = jax.vmap(lambda own, number: assign_block(jax.random.fold_in(keys[6], 2), own, number, TOK_DEV, EXPERTS, TOP, CAP, 2))(routes_keys, routes_turns).reshape((TOKENS, TOP))
    route_weight = jnp.clip(0.2 + 1.3 * jax.random.uniform(keys[7], (TOKENS, TOP), jnp.float32) ** block_scale(keys[7], (TOKENS, TOP), ((0, 8),), -0.2, 0.2), 0.2, 1.5)
    gate_weight = centred(keys[8], (EXPERTS, D, FF), D ** -0.5, 0.125, ((0, 8), (2, 4)))
    up_weight = centred(keys[9], (EXPERTS, D, FF), D ** -0.5, 0.125, ((0, 8), (2, 4)))
    down_weight = centred(keys[10], (EXPERTS, FF, D), FF ** -0.5, 0.1875, ((0, 8), (1, 4)))
    out_weight = centred(keys[11], (D, VW), VW ** -0.5, 0.125, ((1, 4),))
    return dict(hidden=hidden, cotangent=cotangent, retained=retained, queries=queries, key_rows=key_rows, value_rows=value_rows, routes=routes, route_weight=route_weight, gate_weight=gate_weight, up_weight=up_weight, down_weight=down_weight, out_weight=out_weight)


def expert_backward(inputs, upstream, gate_matrix, up_matrix, down_matrix):
    gate_pre = jnp.dot(inputs, gate_matrix, preferred_element_type=jnp.float32)
    up_pre = jnp.dot(inputs, up_matrix, preferred_element_type=jnp.float32)
    sigma = jax.nn.sigmoid(gate_pre)
    active = gate_pre * sigma
    product = (active * up_pre).astype(jnp.bfloat16)
    down_part = jnp.dot(product.T, upstream, preferred_element_type=jnp.float32)
    unit_grad = jnp.dot(upstream, down_matrix.T, preferred_element_type=jnp.float32)
    gate_term = (unit_grad * up_pre * sigma * (1.0 + gate_pre * (1.0 - sigma))).astype(jnp.bfloat16)
    up_term = (unit_grad * active).astype(jnp.bfloat16)
    gate_part = jnp.dot(inputs.T, gate_term, preferred_element_type=jnp.float32)
    up_part = jnp.dot(inputs.T, up_term, preferred_element_type=jnp.float32)
    rows = gate_term.shape[0]
    group = FF // N_TP
    gate_split = gate_term.astype(jnp.float32).reshape(rows, N_TP, group)
    up_split = up_term.astype(jnp.float32).reshape(rows, N_TP, group)
    gate_cols = gate_matrix.astype(jnp.float32).reshape(D, N_TP, group)
    up_cols = up_matrix.astype(jnp.float32).reshape(D, N_TP, group)
    row_part = jnp.einsum('rnf,dnf->nrd', gate_split, gate_cols) + jnp.einsum('rnf,dnf->nrd', up_split, up_cols)
    return (gate_part, up_part, down_part, row_part.astype(jnp.bfloat16))

def slot_targets(routes):
    flat = routes.reshape(N_SP, TOK_DEV * TOP)
    onehot = (flat[:, :, None] == jnp.arange(EXPERTS, dtype=jnp.int32)[None, None, :]).astype(jnp.int32)
    rank = lax.optimization_barrier(jnp.sum(jnp.cumsum(onehot, axis=1) * onehot, axis=2)) - 1
    block = jnp.arange(N_SP, dtype=jnp.int32)[:, None]
    return (flat * (N_SP * CAP) + block * CAP + rank).reshape(-1).astype(jnp.int32)

def head_rates(head_ids, total_tokens):
    ids = head_ids.astype(jnp.float32)
    exponent = jnp.where(2 * head_ids < H, -5.0 - ids, -math.log2(total_tokens) - (ids - H // 2))
    log_gamma = jnp.log1p(-jnp.exp2(exponent))
    scale = jnp.sqrt(-jnp.expm1(2.0 * log_gamma))
    return (log_gamma, scale)

def span_states(query_three, key_three, value_three, output_grad_three, log_gamma):
    count = query_three.shape[0]
    place = jnp.arange(count, dtype=jnp.float32)[:, None]
    suffix_decay = jnp.exp(log_gamma[None, :] * (count - place))
    prefix_decay = jnp.exp(log_gamma[None, :] * (place + 1.0))
    head_position = lax.Precision.HIGHEST
    forward_sweep = jnp.einsum('ibz,ibm->bzm', key_three.astype(jnp.float32) * suffix_decay[:, :, None], value_three.astype(jnp.float32), precision=head_position)
    backward_sweep = jnp.einsum('stz,stb->tzb', query_three.astype(jnp.float32) * prefix_decay[:, :, None], output_grad_three.astype(jnp.float32), precision=head_position)
    return (forward_sweep, backward_sweep)

def span_grads(query_three, key_three, value_three, output_grad_three, prior_positions, later_positions, log_gamma, scale):
    count = query_three.shape[0]
    head_position = lax.Precision.HIGHEST
    query_flat, key_flat, value_flat, output_grad_flat = (query_three.astype(jnp.float32), key_three.astype(jnp.float32), value_three.astype(jnp.float32), output_grad_three.astype(jnp.float32))
    place = jnp.arange(count, dtype=jnp.float32)
    gap = place[:, None] - place[None, :]
    weight = jnp.where(gap[None] >= 0, scale[:, None, None] * jnp.exp(log_gamma[:, None, None] * jnp.maximum(gap, 0.0)[None]), 0.0)
    local_value_grad = (jnp.einsum('ihv,jhv->hij', output_grad_flat, value_flat) * weight).astype(jnp.bfloat16).astype(jnp.float32)
    local_query_key = (jnp.einsum('ihd,jhd->hij', query_flat, key_flat) * weight).astype(jnp.bfloat16).astype(jnp.float32)
    leading_span = (scale[None, :] * jnp.exp(log_gamma[None, :] * place[:, None]))[:, :, None]
    trailing_span = (scale[None, :] * jnp.exp(log_gamma[None, :] * (count - 1.0 - place[:, None])))[:, :, None]
    query_piece = jnp.einsum('zby,yze->bze', local_value_grad, key_flat) + leading_span * jnp.einsum('eal,gel->gea', prior_positions, output_grad_flat, precision=head_position)
    key_piece = jnp.einsum('lcx,clo->xlo', local_value_grad, query_flat) + trailing_span * jnp.einsum('gta,wga->wgt', later_positions, value_flat, precision=head_position)
    value_piece = jnp.einsum('upb,puk->buk', local_query_key, output_grad_flat) + trailing_span * jnp.einsum('tdx,btd->btx', later_positions, key_flat, precision=head_position)
    return (query_piece, key_piece, value_piece)

def reference(hidden, cotangent, retained, queries, key_rows, value_rows, routes, route_weight, gate_weight, up_weight, down_weight, out_weight):
    target = slot_targets(routes)
    slots = EXPERTS * N_SP * CAP
    upstream = (route_weight[:, :, None] * cotangent[:, None, :].astype(jnp.float32)).astype(jnp.bfloat16).reshape(-1, D)
    inputs = jnp.repeat(hidden, TOP, axis=0)
    up_buffer = jnp.zeros((slots, D), jnp.bfloat16).at[target].set(upstream).reshape(EXPERTS, N_SP * CAP, D)
    in_buffer = jnp.zeros((slots, D), jnp.bfloat16).at[target].set(inputs).reshape(EXPERTS, N_SP * CAP, D)
    gate_grad, up_grad, down_grad, row_grad = lax.map(lambda item: expert_backward(*item), (in_buffer, up_buffer, gate_weight, up_weight, down_weight))
    row_sum = lax.optimization_barrier(jnp.sum(row_grad.astype(jnp.float32), axis=1))
    routed = row_sum.reshape(slots, D)[target].reshape(TOKENS, TOP, D).sum(axis=1)
    layer_grad = (cotangent.astype(jnp.float32) + routed).astype(jnp.bfloat16)
    proj_grad = jnp.dot(layer_grad.T, retained, preferred_element_type=jnp.float32)
    mixed_grad = jnp.dot(layer_grad, out_weight, preferred_element_type=jnp.float32).astype(jnp.bfloat16)
    log_gamma, scale = head_rates(jnp.arange(H, dtype=jnp.int32), TOKENS)
    q5 = queries.reshape(N_SP, TOK_DEV, H, DK)
    k5 = key_rows.reshape(N_SP, TOK_DEV, H, DK)
    v5 = value_rows.reshape(N_SP, TOK_DEV, H, DV)
    do5 = mixed_grad.reshape(N_SP, TOK_DEV, H, DV)
    forward_shard_local, backward_local = lax.map(lambda item: span_states(*item, log_gamma), (q5, k5, v5, do5))
    decay_span = jnp.exp(log_gamma * TOK_DEV)[:, None, None]

    def carry_step(carry, local):
        return (carry * decay_span + local, carry)
    empty = jnp.zeros((H, DK, DV), jnp.float32)
    _, before_all = lax.scan(carry_step, empty, forward_shard_local)
    _, after_all = lax.scan(carry_step, empty, backward_local, reverse=True)
    query_gradient, key_gradient, value_gradient = lax.map(lambda item: span_grads(*item, log_gamma, scale), (q5, k5, v5, do5, before_all, after_all))
    return (gate_grad, up_grad, down_grad, proj_grad, query_gradient.reshape(TOKENS, H * DK), key_gradient.reshape(TOKENS, H * DK), value_gradient.reshape(TOKENS, H * DV))
```

```python
import math

import jax
import jax.numpy as jnp
from jax import lax
from jax.sharding import PartitionSpec as P

H = 4
DK = 256
DV = 512


ROWS = (((0,), (0,)), ((), ()))
COLS = (((1,), (1,)), ((), ()))
F32 = jnp.float32
BF16 = jnp.bfloat16


def head_rates(head_ids, total_tokens):
    ids = head_ids.astype(F32)
    exponent = jnp.where(2 * head_ids < H, -5.0 - ids, -math.log2(total_tokens) - (ids - H // 2))
    log_gamma = jnp.log1p(-jnp.exp2(exponent))
    scale = jnp.sqrt(-jnp.expm1(2.0 * log_gamma))
    return (log_gamma, scale)


def swap(x, axis, bits):
    return lax.ppermute(x, axis, [(i, i ^ bits) for i in range(lax.axis_size(axis))])


def exchange(blocks):
    return [blocks[0]] + [swap(block, "sp", k) for k, block in enumerate(blocks) if k]


def gather_tp(x):
    pieces = {0: x}
    bit = lax.axis_size("tp") // 2
    while bit:
        pieces.update({k | bit: swap(piece, "tp", bit) for k, piece in pieces.items()})
        bit //= 2
    return [pieces[k] for k in range(lax.axis_size("tp"))]


def scatter_tp(pieces):
    bit = 1
    pieces = dict(enumerate(pieces))
    while len(pieces) > 1:
        sent = {k ^ bit: swap(piece.astype(BF16), "tp", bit) for k, piece in pieces.items() if k & bit}
        pieces = {k: pieces[k].astype(F32) + sent[k].astype(F32) for k in sent}
        bit *= 2
    return pieces[0]


def block_rows(x, index, size):
    return lax.dynamic_slice_in_dim(x, index * size, size, 0)


def dot(a, b, dims=None):
    if dims is None:
        return jnp.dot(a, b, preferred_element_type=F32)
    return lax.dot_general(a, b, dims, preferred_element_type=F32)


def carry_over(state, span, reverse):
    count = lax.axis_size("sp")
    place = lax.axis_index("sp")
    inner = 2
    outer = count // inner
    low = place % inner
    ahead = (inner - 1 - low) if reverse else low
    sent = state.astype(BF16)
    sign = -1 if reverse else 1
    own = jnp.zeros_like(state)
    other = jnp.where(ahead == 0, 1.0, 0.0) * state
    for d in range(1, outer):
        move = [(i, i + sign * d * inner) for i in range(count) if 0 <= i + sign * d * inner < count]
        got = lax.ppermute(sent, "sp", move).astype(F32)
        own = own + jnp.exp(span * (inner * d - 1)) * got
        other = other + jnp.exp(span * jnp.where(ahead == 0, inner * d, inner * d - 2)) * got
    return own + swap(other.astype(BF16), "sp", 1).astype(F32)


def gather_sp(x):
    count = lax.axis_size("sp")
    even = {k: swap(x, "sp", k) if k else x for k in range(0, count, 2)}
    odd = {k | 1: swap(piece, "sp", 1) for k, piece in even.items()}
    even.update(odd)
    return [even[k] for k in range(count)]


def local(
    hidden,
    cotangent,
    retained,
    queries,
    key_rows,
    value_rows,
    routes,
    route_weight,
    gate_weight,
    up_weight,
    down_weight,
    out_weight,
):
    sp_count = lax.axis_size("sp")
    tp_count = lax.axis_size("tp")
    sp_place = lax.axis_index("sp")
    tp_place = lax.axis_index("tp")
    tokens, width = hidden.shape
    top = routes.shape[1]
    capacity = 3 * tokens * top // (2 * sp_count)
    slots = sp_count * capacity
    col_width = width // tp_count
    gate, up, down = gate_weight[0], up_weight[0], down_weight[0]

    flat = routes.T.reshape(-1)
    order = jnp.arange(flat.shape[0], dtype=jnp.int32)
    before = (flat[None, :] == flat[:, None]) & (order[None, :] < order[:, None])
    rank = jnp.sum(before.astype(jnp.int32), axis=1)
    target = ((flat ^ sp_place) * capacity + rank).reshape(top, tokens)
    place_of = jnp.arange(slots, dtype=jnp.int32)[:, None]
    picks = [(place_of == target[r][None, :]).astype(BF16) for r in range(top)]
    pick_all = sum(picks[1:], picks[0])
    hid_cols = lax.dynamic_slice_in_dim(hidden, tp_place * col_width, col_width, 1)
    cot_cols = lax.dynamic_slice_in_dim(cotangent, tp_place * col_width, col_width, 1)
    cot_wide = cot_cols.astype(F32)
    upstream = jnp.concatenate(
        [(route_weight[:, r : r + 1] * cot_wide).astype(BF16) for r in range(top)], axis=0
    )
    in_send = dot(pick_all, hid_cols).astype(BF16).reshape(sp_count, capacity, col_width)
    up_send = (
        dot(jnp.concatenate(picks, axis=1), upstream)
        .astype(BF16)
        .reshape(sp_count, capacity, col_width)
    )
    got_in = jnp.concatenate(exchange([in_send[k] for k in range(sp_count)]), axis=0)
    got_up = jnp.concatenate(exchange([up_send[k] for k in range(sp_count)]), axis=0)
    ins = gather_tp(got_in)
    ups = gather_tp(got_up)

    blocks = [tp_place ^ k for k in range(tp_count)]
    gates = [block_rows(gate, b, col_width) for b in blocks]
    upws = [block_rows(up, b, col_width) for b in blocks]
    downs = [lax.dynamic_slice_in_dim(down, b * col_width, col_width, 1) for b in blocks]
    gate_pre = sum(dot(x, w) for x, w in zip(ins, gates))
    up_pre = sum(dot(x, w) for x, w in zip(ins, upws))
    sigma = jax.nn.sigmoid(gate_pre)
    active = gate_pre * sigma
    product = (active * up_pre).astype(BF16)
    unit_grad = sum(dot(x, w, COLS) for x, w in zip(ups, downs))
    gate_term = (unit_grad * up_pre * sigma * (1.0 + gate_pre * (1.0 - sigma))).astype(BF16)
    up_term = (unit_grad * active).astype(BF16)
    row_parts = [
        (dot(gate_term, g, COLS) + dot(up_term, u, COLS)).astype(BF16) for g, u in zip(gates, upws)
    ]
    row_grad = scatter_tp(row_parts).astype(BF16).reshape(sp_count, capacity, col_width)
    returned = jnp.concatenate(exchange([row_grad[k] for k in range(sp_count)]), axis=0)
    routed = dot(pick_all, returned, ROWS)
    layer_cols = (cot_wide + routed).astype(BF16)

    gate_grad = jnp.zeros((width, gate.shape[1]), F32)
    up_grad = jnp.zeros((width, gate.shape[1]), F32)
    down_grad = jnp.zeros((gate.shape[1], width), F32)
    for k, b in enumerate(blocks):
        gate_grad = lax.dynamic_update_slice_in_dim(
            gate_grad, dot(ins[k], gate_term, ROWS), b * col_width, 0
        )
        up_grad = lax.dynamic_update_slice_in_dim(
            up_grad, dot(ins[k], up_term, ROWS), b * col_width, 0
        )
        down_grad = lax.dynamic_update_slice_in_dim(
            down_grad, dot(product, ups[k], ROWS), b * col_width, 1
        )

    layers = gather_tp(layer_cols)
    mixed_grad = sum(
        dot(x, block_rows(out_weight, b, col_width)) for x, b in zip(layers, blocks)
    ).astype(BF16)

    kept = gather_sp(retained)
    part = width // sp_count
    layer_all = jnp.zeros((tokens, width), BF16)
    for x, b in zip(layers, blocks):
        layer_all = lax.dynamic_update_slice_in_dim(layer_all, x, b * col_width, 1)
    half = part // 2
    core = tp_place % 2
    layer_split = layer_all.reshape(tokens, sp_count, 2, half)
    layer_split = lax.dynamic_index_in_dim(layer_split, core, 2, False)
    layer_send = [
        lax.dynamic_index_in_dim(layer_split, sp_place ^ k, 1, False) for k in range(sp_count)
    ]
    mine = jnp.concatenate(exchange(layer_send), axis=0)
    theirs = swap(mine, "tp", 1)
    kept_all = jnp.concatenate(kept, axis=0)
    low = jnp.where(core == 0, mine, theirs)
    high = jnp.where(core == 0, theirs, mine)
    proj_grad = dot(jnp.concatenate([low, high], axis=1), kept_all, ROWS)

    log_gamma, scale = head_rates(tp_place, tokens * sp_count)
    place = jnp.arange(tokens, dtype=F32)
    span = log_gamma * tokens
    suffix_decay = jnp.exp(log_gamma * (tokens - place))[:, None]
    prefix_decay = jnp.exp(log_gamma * (place + 1.0))[:, None]
    key_decayed = (key_rows.astype(F32) * suffix_decay).astype(BF16)
    query_decayed = (queries.astype(F32) * prefix_decay).astype(BF16)
    prior = carry_over(dot(key_decayed, value_rows, ROWS), span, False).astype(BF16)
    later = carry_over(dot(query_decayed, mixed_grad, ROWS), span, True).astype(BF16)
    gap = place[:, None] - place[None, :]
    weight = jnp.where(gap >= 0, scale * jnp.exp(log_gamma * jnp.maximum(gap, 0.0)), 0.0)
    near_dv = (dot(mixed_grad, value_rows, COLS) * weight).astype(BF16)
    near_qk = (dot(queries, key_rows, COLS) * weight).astype(BF16)
    leading = (scale * jnp.exp(log_gamma * place))[:, None]
    trailing = (scale * jnp.exp(log_gamma * (tokens - 1.0 - place)))[:, None]
    query_gradient = dot(near_dv, key_rows) + leading * dot(mixed_grad, prior, COLS)
    key_gradient = dot(near_dv, queries, ROWS) + trailing * dot(value_rows, later, COLS)
    value_gradient = dot(near_qk, mixed_grad, ROWS) + trailing * dot(key_rows, later)
    return (
        gate_grad[None],
        up_grad[None],
        down_grad[None],
        proj_grad,
        query_gradient,
        key_gradient,
        value_gradient,
    )


def solution(mesh):
    return jax.shard_map(
        local,
        mesh=mesh,
        in_specs=(
            P("sp", None),
            P("sp", None),
            P("sp", "tp"),
            P("sp", "tp"),
            P("sp", "tp"),
            P("sp", "tp"),
            P("sp", None),
            P("sp", None),
            P("sp", None, "tp"),
            P("sp", None, "tp"),
            P("sp", "tp", None),
            P(None, "tp"),
        ),
        out_specs=(
            P("sp", None, "tp"),
            P("sp", None, "tp"),
            P("sp", "tp", None),
            P("sp", "tp"),
            P("sp", "tp"),
            P("sp", "tp"),
            P("sp", "tp"),
        ),
        check_vma=False,
    )
```

```python
import math

import jax
import jax.numpy as jnp
from jax import lax
from jax.experimental import pallas as pl
from jax.experimental.pallas import tpu as pltpu
from jax.sharding import PartitionSpec as P


H = 4


ROWS = (((0,), (0,)), ((), ()))
COLS = (((1,), (1,)), ((), ()))
F32 = jnp.float32
BF16 = jnp.bfloat16


def head_rates(head_ids, total_tokens):
    ids = head_ids.astype(F32)
    exponent = jnp.where(2 * head_ids < H, -5.0 - ids, -math.log2(total_tokens) - (ids - H // 2))
    log_gamma = jnp.log1p(-jnp.exp2(exponent))
    scale = jnp.sqrt(-jnp.expm1(2.0 * log_gamma))
    return (log_gamma, scale)


def swap(x, axis, bits):
    return lax.ppermute(x, axis, [(i, i ^ bits) for i in range(lax.axis_size(axis))])


def far_first(count):
    return sorted(range(1, count), key=lambda k: (-(k & (count // 2)), k))


def exchange(blocks):
    count = blocks.shape[0]
    got = {k: swap(blocks[k], "sp", k) for k in far_first(count)}
    return [got[k] for k in range(1, count)]


def transpose_blocks(x):
    return lax.all_to_all(x, "sp", split_axis=0, concat_axis=0, tiled=True)


def join_body(own_ref, *refs):
    pieces, out_ref = refs[:-1], refs[-1]
    out_ref[0] = own_ref[0]
    for k, piece in enumerate(pieces, 1):
        out_ref[k] = piece[...]


def join(own, pieces):
    (out,) = call(join_body, ((own.shape, own.dtype),), own, *pieces, work=own.size * 256)
    return out


def gather_tp(x):
    pieces = {0: x}
    bit = lax.axis_size("tp") // 2
    while bit:
        pieces.update({k | bit: swap(p, "tp", bit) for k, p in pieces.items()})
        bit //= 2
    return [pieces[k] for k in range(lax.axis_size("tp"))]


def scatter_tp(pieces):
    bit = 1
    pieces = dict(enumerate(pieces))
    while len(pieces) > 1:
        sent = {
            k ^ bit: swap(p.astype(BF16), "tp", bit)
            for k, p in pieces.items()
            if k & bit
        }
        pieces = {k: pieces[k].astype(F32) + sent[k].astype(F32) for k in sent}
        bit *= 2
    return pieces[0]


def flops(count):
    return pl.CostEstimate(flops=int(count), bytes_accessed=0, transcendentals=0)


def call(body, outs, *args, scalars=(), work=0):
    vmem = pl.BlockSpec(memory_space=pltpu.VMEM)
    smem = pl.BlockSpec(memory_space=pltpu.SMEM)
    return pl.pallas_call(
        body,
        in_specs=[smem] * len(scalars) + [vmem] * len(args),
        out_specs=[vmem] * len(outs),
        out_shape=[jax.ShapeDtypeStruct(shape, kind) for shape, kind in outs],
        cost_estimate=flops(work),
    )(*scalars, *args)


def layer_body(pick_ref, own_ref, *refs):
    pieces, (cot_ref, layer_ref) = refs[:-2], refs[-2:]
    total = dot(pick_ref[0], own_ref[0], ROWS)
    for k, piece in enumerate(pieces, 1):
        total = total + dot(pick_ref[k], piece[...], ROWS)
    layer_ref[...] = (cot_ref[...].astype(F32) + total).astype(BF16)


def mix_body(place_ref, *refs):
    pieces, (weight_ref, query_ref, send_ref, mixed_ref, state_ref) = refs[:-5], refs[-5:]
    place = place_ref[0]
    cols = pieces[0].shape[1]
    half = send_ref.shape[2]
    count = send_ref.shape[0] // len(pieces)
    total = None
    for k, piece in enumerate(pieces):
        block = place ^ k
        x = piece[...]
        for q in range(count):
            low = x[:, 2 * q * half : (2 * q + 1) * half]
            high = x[:, (2 * q + 1) * half : (2 * q + 2) * half]
            send_ref[block * count + q] = jnp.where(place % 2 == 0, low, high)
        part = dot(x, weight_ref[pl.ds(block * cols, cols), :])
        total = part if total is None else total + part
    mixed = total.astype(BF16)
    mixed_ref[...] = mixed
    state_ref[...] = dot(query_ref[...], mixed, ROWS).astype(BF16)


def decays(rates_ref, count):
    place = lax.broadcasted_iota(jnp.int32, (count, 1), 0).astype(F32)
    leading = rates_ref[1] * jnp.exp(rates_ref[0] * place)
    trailing = rates_ref[1] * jnp.exp(rates_ref[0] * (count - 1.0 - place))
    return leading, trailing


def paired(low, own_ref, got_ref):
    own, got = own_ref[...], got_ref[...]
    return jnp.concatenate([jnp.where(low, own, got), jnp.where(low, got, own)])


def near_body(ids_ref, rates_ref, mixed_ref, query_ref, key_ref, value_ref, own_ref, got_ref, *outs):
    count = mixed_ref.shape[0]
    mixed, query, key = mixed_ref[...], query_ref[...], key_ref[...]
    row = lax.broadcasted_iota(jnp.int32, (count, count), 0)
    col = lax.broadcasted_iota(jnp.int32, (count, count), 1)
    gap = (row - col).astype(F32)
    weight = rates_ref[1] * jnp.exp(rates_ref[0] * jnp.maximum(gap, 0.0))
    weight = jnp.where(gap >= 0.0, weight, 0.0)
    near_dv = (dot(mixed, value_ref[...], COLS) * weight).astype(BF16)
    near_qk = (dot(query, key, COLS) * weight).astype(BF16)
    prior = paired(ids_ref[1] % 2 == 0, own_ref, got_ref)
    leading, _ = decays(rates_ref, count)
    query_ref, key_near_ref, value_near_ref = outs
    query_ref[...] = dot(near_dv, key) + leading * dot(mixed, prior, COLS)
    key_near_ref[...] = dot(near_dv, query, ROWS)
    value_near_ref[...] = dot(near_qk, mixed, ROWS)


def last_body(ids_ref, rates_ref, own_ref, got_ref, key_ref, value_ref, kn_ref, vn_ref, kg_ref, vg_ref):
    later = paired(ids_ref[1] % 2 == 0, own_ref, got_ref)
    _, trailing = decays(rates_ref, key_ref.shape[0])
    kg_ref[...] = kn_ref[...] + trailing * dot(value_ref[...], later, COLS)
    vg_ref[...] = vn_ref[...] + trailing * dot(key_ref[...], later)


def pre_body(place_ref, *refs):
    pieces = (len(refs) - 2) // 3
    ins, gates, ups = refs[:pieces], refs[pieces : 2 * pieces], refs[2 * pieces : 3 * pieces]
    refs[-2][...] = sum(dot(x[...], w[...]) for x, w in zip(ins, gates))
    refs[-1][...] = sum(dot(x[...], w[...]) for x, w in zip(ins, ups))


def pre_call(place, ins, gate, up):
    slots, cols = ins[0].shape
    units = gate.shape[1]
    pieces = len(ins)
    step = math.gcd(slots, 256)
    row = lambda width: pl.BlockSpec((step, width), lambda i, s: (i, 0))
    weights = [
        pl.BlockSpec((cols, units), lambda i, s, k=k: (s[0] ^ k, 0)) for k in range(pieces)
    ]
    return pl.pallas_call(
        pre_body,
        grid_spec=pltpu.PrefetchScalarGridSpec(
            num_scalar_prefetch=1,
            grid=(slots // step,),
            in_specs=[row(cols)] * pieces + weights * 2,
            out_specs=[row(units)] * 2,
        ),
        out_shape=[jax.ShapeDtypeStruct((slots, units), F32)] * 2,
        cost_estimate=flops(4 * slots * cols * units * pieces),
    )(place, *ins, *[gate] * pieces, *[up] * pieces)


def grad_body(place_ref, *refs):
    place = place_ref[0]
    pieces = (len(refs) - 6) // 2
    ins, ups = refs[:pieces], refs[pieces : 2 * pieces]
    gate_ref, up_ref, product_ref, gate_out, up_out, down_out = refs[2 * pieces :]
    gate_term, up_term, product = gate_ref[...], up_ref[...], product_ref[...]
    for k in range(pieces):
        x = ins[k][...]
        gate_out[place ^ k] = dot(x, gate_term, ROWS)
        up_out[place ^ k] = dot(x, up_term, ROWS)
    width = ups[0].shape[1]
    total = width * pl.num_programs(0)
    for k in range(pieces):
        start = (place ^ k) * total + pl.program_id(0) * width
        start = pl.multiple_of(start, width)
        down_out[:, pl.ds(start, width)] = dot(product, ups[k][...], ROWS)


def grad_call(place, ins, ups, gate_term, up_term, product):
    slots, cols = ins[0].shape
    units = product.shape[1]
    pieces = len(ins)
    step = math.gcd(cols, 256)
    col = pl.BlockSpec((slots, step), lambda i, s: (0, i))
    whole = pl.BlockSpec((slots, units), lambda i, s: (0, 0))
    out = pl.BlockSpec((pieces, step, units), lambda i, s: (0, i, 0))
    gate_grad, up_grad, down_grad = pl.pallas_call(
        grad_body,
        grid_spec=pltpu.PrefetchScalarGridSpec(
            num_scalar_prefetch=1,
            grid=(cols // step,),
            in_specs=[col] * (2 * pieces) + [whole] * 3,
            out_specs=[out, out, pl.BlockSpec((units, pieces * cols), lambda i, s: (0, 0))],
        ),
        out_shape=[jax.ShapeDtypeStruct((pieces, cols, units), F32)] * 2
        + [jax.ShapeDtypeStruct((units, pieces * cols), F32)],
        cost_estimate=flops(6 * slots * cols * units * pieces),
    )(place, *ins, *ups, gate_term, up_term, product)
    width = pieces * cols
    return gate_grad.reshape(width, units), up_grad.reshape(width, units), down_grad


def expert_body(place_ref, *refs):
    ups, downs = refs[0:2], refs[2:4]
    partial_ref, gate_pre_ref, up_pre_ref = refs[4:7]
    outs = (len(refs) - 10) // 3
    gates, upws = refs[7 : 7 + outs], refs[7 + outs : 7 + 2 * outs]
    product_ref, gate_term_ref, up_term_ref = refs[7 + 2 * outs : 10 + 2 * outs]
    rows = refs[10 + 2 * outs :]
    unit_grad = partial_ref[...]
    for x, w in zip(ups, downs):
        unit_grad = unit_grad + dot(x[...], w[...], COLS)
    gate_pre = gate_pre_ref[...]
    up_pre = up_pre_ref[...]
    sigma = jax.nn.sigmoid(gate_pre)
    active = gate_pre * sigma
    product_ref[...] = (active * up_pre).astype(BF16)
    gate_term = (unit_grad * up_pre * sigma * (1.0 + gate_pre * (1.0 - sigma))).astype(BF16)
    up_term = (unit_grad * active).astype(BF16)
    gate_term_ref[...] = gate_term
    up_term_ref[...] = up_term
    for g, u, out in zip(gates, upws, rows):
        out[...] = (dot(gate_term, g[...], COLS) + dot(up_term, u[...], COLS)).astype(BF16)


def expert_call(place, ups, partial, gate_pre, up_pre, down, gate, up):
    slots, cols = ups[0].shape
    units = gate.shape[1]
    pieces = gate.shape[0] // cols
    step = math.gcd(slots, 256)
    row = lambda width: pl.BlockSpec((step, width), lambda i, s: (i, 0))
    down_of = lambda k: pl.BlockSpec((units, cols), lambda i, s, k=k: (0, s[0] ^ k))
    weight_of = lambda k: pl.BlockSpec((cols, units), lambda i, s, k=k: (s[0] ^ k, 0))
    weights = [weight_of(k) for k in range(pieces)]
    return pl.pallas_call(
        expert_body,
        grid_spec=pltpu.PrefetchScalarGridSpec(
            num_scalar_prefetch=1,
            grid=(slots // step,),
            in_specs=[row(cols)] * 2
            + [down_of(pieces - 2), down_of(pieces - 1)]
            + [row(units)] * 3
            + weights
            + weights,
            out_specs=[row(units)] * 3 + [row(cols)] * pieces,
        ),
        out_shape=[jax.ShapeDtypeStruct((slots, units), BF16)] * 3
        + [jax.ShapeDtypeStruct((slots, cols), BF16)] * pieces,
        cost_estimate=flops(6 * slots * cols * units * pieces),
    )(place, *ups, down, down, partial, gate_pre, up_pre, *[gate] * pieces, *[up] * pieces)


def proj_body(place_ref, mine_ref, theirs_ref, even_ref, odd_ref, out_ref):
    place = place_ref[1]
    core = place_ref[0] % 2
    for rows_ref, slot in ((mine_ref, core), (theirs_ref, 1 - core)):
        total = None
        for k in range(even_ref.shape[0]):
            for kept_ref, low in ((even_ref, 0), (odd_ref, 1)):
                part = dot(rows_ref[place ^ (2 * k + low)], kept_ref[k], ROWS)
                total = part if total is None else total + part
        out_ref[slot] = total


def dot(a, b, dims=None):
    if dims is None:
        return jnp.dot(a, b, preferred_element_type=F32)
    return lax.dot_general(a, b, dims, preferred_element_type=F32)


def carry_pair(state, span, reverse):
    low = lax.axis_index("sp") % 2
    first = (low == 1) if reverse else (low == 0)
    half = state.shape[0] // 2
    mine = lax.dynamic_slice_in_dim(state, low * half, half, 0)
    theirs = swap(lax.dynamic_slice_in_dim(state, (1 - low) * half, half, 0), "sp", 1)
    mine, theirs = mine.astype(F32), theirs.astype(F32)
    early = jnp.where(first, mine, theirs)
    late = jnp.where(first, theirs, mine)
    return early, (late + jnp.exp(span) * early).astype(BF16)


def carry_outer(total, reverse):
    count = lax.axis_size("sp")
    sign = -2 if reverse else 2
    return [
        lax.ppermute(
            total, "sp", [(i, i + sign * d) for i in range(count) if 0 <= i + sign * d < count]
        )
        for d in range(1, count // 2)
    ]


def carry_inner(early, outer, span, reverse):
    low = lax.axis_index("sp") % 2
    first = (low == 1) if reverse else (low == 0)
    ahead = jnp.zeros(early.shape, F32)
    for d, piece in enumerate(outer, 1):
        ahead = ahead + jnp.exp(span * (2 * d - 2)) * piece.astype(F32)
    behind = early + jnp.exp(span) * ahead
    own = jnp.where(first, ahead, behind).astype(BF16)
    return own, jnp.where(first, behind, ahead).astype(BF16)


def local(
    hidden,
    cotangent,
    retained,
    queries,
    key_rows,
    value_rows,
    routes,
    route_weight,
    gate_weight,
    up_weight,
    down_weight,
    out_weight,
):
    sp_count = lax.axis_size("sp")
    tp_count = lax.axis_size("tp")
    sp_place = lax.axis_index("sp")
    tp_place = lax.axis_index("tp")
    tokens, width = hidden.shape
    ids = jnp.stack([tp_place, sp_place])
    rates = jnp.stack(head_rates(tp_place, tokens * sp_count))
    log_gamma = rates[0]
    top = routes.shape[1]
    capacity = 3 * tokens * top // (2 * sp_count)
    slots = sp_count * capacity
    col_width = width // tp_count
    gate, up, down = gate_weight[0], up_weight[0], down_weight[0]

    flat = routes.T.reshape(-1)
    order = jnp.arange(flat.shape[0], dtype=jnp.int32)
    before = (flat[None, :] == flat[:, None]) & (order[None, :] < order[:, None])
    rank = jnp.sum(before.astype(jnp.int32), axis=1)
    target = ((flat ^ sp_place) * capacity + rank).reshape(top, tokens)
    place_of = jnp.arange(slots, dtype=jnp.int32)[:, None]
    picks = [(place_of == target[r][None, :]).astype(BF16) for r in range(top)]
    pick_all = sum(picks[1:], picks[0])
    hid_cols = lax.dynamic_slice_in_dim(hidden, tp_place * col_width, col_width, 1)
    cot_cols = lax.dynamic_slice_in_dim(cotangent, tp_place * col_width, col_width, 1)
    cot_wide = cot_cols.astype(F32)
    upstream = jnp.concatenate(
        [(route_weight[:, r : r + 1] * cot_wide).astype(BF16) for r in range(top)], axis=0
    )
    in_send = dot(pick_all, hid_cols).astype(BF16).reshape(sp_count, capacity, col_width)
    up_send = (
        dot(jnp.concatenate(picks, axis=1), upstream)
        .astype(BF16)
        .reshape(sp_count, capacity, col_width)
    )
    got_in = join(in_send, exchange(in_send)).reshape(slots, col_width)
    got_up = join(up_send, exchange(up_send)).reshape(slots, col_width)
    place = jnp.arange(tokens, dtype=F32)
    span = log_gamma * tokens
    suffix_decay = jnp.exp(log_gamma * (tokens - place))[:, None]
    prefix_decay = jnp.exp(log_gamma * (place + 1.0))[:, None]
    key_decayed = (key_rows.astype(F32) * suffix_decay).astype(BF16)
    query_decayed = (queries.astype(F32) * prefix_decay).astype(BF16)
    prior_state = dot(key_decayed, value_rows, ROWS).astype(BF16)
    prior_early, prior_total = carry_pair(prior_state, span, False)
    ins = gather_tp(got_in)
    ups = gather_tp(got_up)
    kept = [retained] + [swap(retained, "sp", k) for k in range(2, sp_count, 2)]
    prior_outer = carry_outer(prior_total, False)
    blocks = [tp_place ^ k for k in range(tp_count)]
    downs = [lax.dynamic_slice_in_dim(down, b * col_width, col_width, 1) for b in blocks[:-2]]
    gate_pre, up_pre = pre_call(ids, ins, gate, up)
    partial = sum(dot(x, w, COLS) for x, w in zip(ups, downs))
    product, gate_term, up_term, *row_parts = expert_call(
        ids, ups[-2:], partial, gate_pre, up_pre, down, gate, up
    )
    row_grad = scatter_tp(row_parts).astype(BF16)
    row_grad = row_grad.reshape(sp_count, capacity, col_width)
    returned = exchange(row_grad)
    even = jnp.stack(kept)
    odd = swap(even, "sp", 1)
    prior_own, prior_sent = carry_inner(prior_early, prior_outer, span, False)
    prior_got = swap(prior_sent, "sp", 1)
    (layer_cols,) = call(
        layer_body,
        (((tokens, col_width), BF16),),
        pick_all.reshape(sp_count, capacity, tokens),
        row_grad,
        *returned,
        cot_cols,
        work=2 * slots * tokens * col_width,
    )

    gate_grad, up_grad, down_grad = grad_call(
        ids, ins, ups, gate_term, up_term, product
    )

    layers = gather_tp(layer_cols)
    half = width // sp_count // 2
    values = value_rows.shape[1]
    layer_send, mixed_grad, state = call(
        mix_body,
        (
            ((sp_count, tokens, half), BF16),
            ((tokens, values), BF16),
            ((queries.shape[1], values), BF16),
        ),
        *layers,
        out_weight,
        query_decayed,
        scalars=(ids,),
        work=2 * tokens * width * values,
    )

    later_early, later_total = carry_pair(state, span, True)
    later_outer = carry_outer(later_total, True)
    mine = transpose_blocks(layer_send)
    later_own, later_sent = carry_inner(later_early, later_outer, span, True)
    later_got = swap(later_sent, "sp", 1)
    theirs = swap(mine, "tp", 1)
    query_gradient, key_near, value_near = call(
        near_body,
        ((queries.shape, F32), (queries.shape, F32), (value_rows.shape, F32)),
        mixed_grad,
        queries,
        key_rows,
        value_rows,
        prior_own,
        prior_got,
        scalars=(ids, rates),
        work=10 * tokens * tokens * values,
    )
    key_gradient, value_gradient = call(
        last_body,
        ((key_near.shape, F32), (value_near.shape, F32)),
        later_own,
        later_got,
        key_rows,
        value_rows,
        key_near,
        value_near,
        scalars=(ids, rates),
        work=4 * tokens * values * queries.shape[1],
    )
    (proj_grad,) = call(
        proj_body,
        (((2, half, retained.shape[1]), F32),),
        mine,
        theirs,
        even,
        odd,
        scalars=(ids,),
        work=2 * sp_count * tokens * 2 * half * retained.shape[1],
    )
    proj_grad = proj_grad.reshape(2 * half, retained.shape[1])
    return (
        gate_grad[None],
        up_grad[None],
        down_grad[None],
        proj_grad,
        query_gradient,
        key_gradient,
        value_gradient,
    )


def solution(mesh):
    return jax.shard_map(
        local,
        mesh=mesh,
        in_specs=(
            P("sp", None),
            P("sp", None),
            P("sp", "tp"),
            P("sp", "tp"),
            P("sp", "tp"),
            P("sp", "tp"),
            P("sp", None),
            P("sp", None),
            P("sp", None, "tp"),
            P("sp", None, "tp"),
            P("sp", "tp", None),
            P(None, "tp"),
        ),
        out_specs=(
            P("sp", None, "tp"),
            P("sp", None, "tp"),
            P("sp", "tp", None),
            P("sp", "tp"),
            P("sp", "tp"),
            P("sp", "tp"),
            P("sp", "tp"),
        ),
        check_vma=False,
    )
```

```python
import math

import jax
import jax.numpy as jnp
from jax import lax
from jax.experimental import pallas as pl
from jax.experimental.pallas import tpu as pltpu
from jax.sharding import PartitionSpec as P


H = 4


ROWS = (((0,), (0,)), ((), ()))
COLS = (((1,), (1,)), ((), ()))
F32 = jnp.float32
BF16 = jnp.bfloat16


def head_rates(head_ids, total_tokens):
    ids = head_ids.astype(F32)
    exponent = jnp.where(2 * head_ids < H, -5.0 - ids, -math.log2(total_tokens) - (ids - H // 2))
    log_gamma = jnp.log1p(-jnp.exp2(exponent))
    scale = jnp.sqrt(-jnp.expm1(2.0 * log_gamma))
    return (log_gamma, scale)


def swap(x, axis, bits):
    return lax.ppermute(x, axis, [(i, i ^ bits) for i in range(lax.axis_size(axis))])


def far_first(count):
    return sorted(range(1, count), key=lambda k: (-(k & (count // 2)), k))


def exchange(blocks):
    count = blocks.shape[0]
    got = {k: swap(blocks[k], "sp", k) for k in far_first(count)}
    return [got[k] for k in range(1, count)]


def transpose_blocks(x):
    return lax.all_to_all(x, "sp", split_axis=0, concat_axis=0, tiled=True)


def join_body(own_ref, *refs):
    pieces, out_ref = refs[:-1], refs[-1]
    out_ref[0] = own_ref[0]
    for k, piece in enumerate(pieces, 1):
        out_ref[k] = piece[...]


def join(own, pieces):
    (out,) = call(join_body, ((own.shape, own.dtype),), own, *pieces, work=own.size * 256)
    return out


def gather_tp(x):
    pieces = {0: x}
    bit = lax.axis_size("tp") // 2
    while bit:
        pieces.update({k | bit: swap(p, "tp", bit) for k, p in pieces.items()})
        bit //= 2
    return [pieces[k] for k in range(lax.axis_size("tp"))]


def scatter_tp(pieces):
    bit = 1
    pieces = dict(enumerate(pieces))
    while len(pieces) > 1:
        sent = {
            k ^ bit: swap(p.astype(BF16), "tp", bit)
            for k, p in pieces.items()
            if k & bit
        }
        pieces = {k: pieces[k].astype(F32) + sent[k].astype(F32) for k in sent}
        bit *= 2
    return pieces[0]


def flops(count):
    return pl.CostEstimate(flops=int(count), bytes_accessed=0, transcendentals=0)


def call(body, outs, *args, scalars=(), work=0, scratch=()):
    vmem = pl.BlockSpec(memory_space=pltpu.VMEM)
    smem = pl.BlockSpec(memory_space=pltpu.SMEM)
    return pl.pallas_call(
        body,
        in_specs=[smem] * len(scalars) + [vmem] * len(args),
        out_specs=[vmem] * len(outs),
        out_shape=[jax.ShapeDtypeStruct(shape, kind) for shape, kind in outs],
        scratch_shapes=[pltpu.VMEM(shape, kind) for shape, kind in scratch],
        cost_estimate=flops(work),
    )(*scalars, *args)


def layer_body(pick_ref, own_ref, *refs):
    pieces, (cot_ref, layer_ref) = refs[:-2], refs[-2:]
    total = dot(pick_ref[0], own_ref[0], ROWS)
    for k, piece in enumerate(pieces, 1):
        total = total + dot(pick_ref[k], piece[...], ROWS)
    layer_ref[...] = (cot_ref[...].astype(F32) + total).astype(BF16)


def mix_body(ids_ref, *refs):
    pieces, (weight_ref, query_ref) = refs[:-6], refs[-6:-4]
    send_ref, mixed_ref, mine_ref, theirs_ref = refs[-4:]
    place = ids_ref[0]
    cols = pieces[0].shape[1]
    count, rows, width = send_ref.shape
    count //= len(pieces)
    total = None
    for k, piece in enumerate(pieces):
        block = place ^ k
        x = piece[pl.ds(place * rows, rows), :]
        for q in range(count):
            send_ref[block * count + q] = x[:, q * width : (q + 1) * width]
        part = dot(piece[...], weight_ref[pl.ds(block * cols, cols), :])
        total = part if total is None else total + part
    mixed = total.astype(BF16)
    mixed_ref[...] = mixed
    state = dot(query_ref[...], mixed, ROWS).astype(BF16)
    half = mine_ref.shape[0]
    low = ids_ref[1] % 2 == 0
    mine_ref[...] = jnp.where(low, state[:half], state[half:])
    theirs_ref[...] = jnp.where(low, state[half:], state[:half])


def decays(rates_ref, count):
    place = lax.broadcasted_iota(jnp.int32, (count, 1), 0).astype(F32)
    leading = rates_ref[1] * jnp.exp(rates_ref[0] * place)
    trailing = rates_ref[1] * jnp.exp(rates_ref[0] * (count - 1.0 - place))
    return leading, trailing


def paired(low, own_ref, got_ref):
    own, got = own_ref[...], got_ref[...]
    return jnp.concatenate([jnp.where(low, own, got), jnp.where(low, got, own)])


def near_body(ids_ref, rates_ref, mixed_ref, query_ref, key_ref, value_ref, own_ref, got_ref, *outs):
    count = mixed_ref.shape[0]
    mixed, query, key = mixed_ref[...], query_ref[...], key_ref[...]
    row = lax.broadcasted_iota(jnp.int32, (count, count), 0)
    col = lax.broadcasted_iota(jnp.int32, (count, count), 1)
    gap = (row - col).astype(F32)
    weight = rates_ref[1] * jnp.exp(rates_ref[0] * jnp.maximum(gap, 0.0))
    weight = jnp.where(gap >= 0.0, weight, 0.0)
    near_dv = (dot(mixed, value_ref[...], COLS) * weight).astype(BF16)
    near_qk = (dot(query, key, COLS) * weight).astype(BF16)
    prior = paired(ids_ref[1] % 2 == 0, own_ref, got_ref)
    leading, _ = decays(rates_ref, count)
    query_ref, key_near_ref, value_near_ref = outs
    query_ref[...] = dot(near_dv, key) + leading * dot(mixed, prior, COLS)
    key_near_ref[...] = dot(near_dv, query, ROWS)
    value_near_ref[...] = dot(near_qk, mixed, ROWS)


def last_body(ids_ref, rates_ref, own_ref, got_ref, key_ref, value_ref, kn_ref, vn_ref, *refs):
    kg_ref, vg_ref = refs[-4:-2]
    later = paired(ids_ref[1] % 2 == 0, own_ref, got_ref)
    _, trailing = decays(rates_ref, key_ref.shape[0])
    kg_ref[...] = kn_ref[...] + trailing * dot(value_ref[...], later, COLS)
    vg_ref[...] = vn_ref[...] + trailing * dot(key_ref[...], later)
    proj_body(ids_ref, *refs[:-4], *refs[-2:])


def pre_body(place_ref, *refs):
    pieces = (len(refs) - 2) // 3
    ins, gates, ups = refs[:pieces], refs[pieces : 2 * pieces], refs[2 * pieces : 3 * pieces]
    refs[-2][...] = sum(dot(x[...], w[...]) for x, w in zip(ins, gates))
    refs[-1][...] = sum(dot(x[...], w[...]) for x, w in zip(ins, ups))


def pre_call(place, ins, gate, up):
    slots, cols = ins[0].shape
    units = gate.shape[1]
    pieces = len(ins)
    step = math.gcd(slots, 256)
    row = lambda width: pl.BlockSpec((step, width), lambda i, s: (i, 0))
    weights = [
        pl.BlockSpec((cols, units), lambda i, s, k=k: (s[0] ^ k, 0)) for k in range(pieces)
    ]
    return pl.pallas_call(
        pre_body,
        grid_spec=pltpu.PrefetchScalarGridSpec(
            num_scalar_prefetch=1,
            grid=(slots // step,),
            in_specs=[row(cols)] * pieces + weights * 2,
            out_specs=[row(units)] * 2,
        ),
        out_shape=[jax.ShapeDtypeStruct((slots, units), F32)] * 2,
        cost_estimate=flops(4 * slots * cols * units * pieces),
    )(place, *ins, *[gate] * pieces, *[up] * pieces)


def grad_body(place_ref, *refs):
    place = place_ref[0]
    pieces = (len(refs) - 6) // 2
    ins, ups = refs[:pieces], refs[pieces : 2 * pieces]
    gate_ref, up_ref, product_ref, gate_out, up_out, down_out = refs[2 * pieces :]
    gate_term, up_term, product = gate_ref[...], up_ref[...], product_ref[...]
    for k in range(pieces):
        x = ins[k][...]
        gate_out[place ^ k] = dot(x, gate_term, ROWS)
        up_out[place ^ k] = dot(x, up_term, ROWS)
    width = ups[0].shape[1]
    total = width * pl.num_programs(0)
    for k in range(pieces):
        start = (place ^ k) * total + pl.program_id(0) * width
        start = pl.multiple_of(start, width)
        down_out[:, pl.ds(start, width)] = dot(product, ups[k][...], ROWS)


def grad_call(place, ins, ups, gate_term, up_term, product):
    slots, cols = ins[0].shape
    units = product.shape[1]
    pieces = len(ins)
    step = math.gcd(cols, 256)
    col = pl.BlockSpec((slots, step), lambda i, s: (0, i))
    whole = pl.BlockSpec((slots, units), lambda i, s: (0, 0))
    out = pl.BlockSpec((pieces, step, units), lambda i, s: (0, i, 0))
    gate_grad, up_grad, down_grad = pl.pallas_call(
        grad_body,
        grid_spec=pltpu.PrefetchScalarGridSpec(
            num_scalar_prefetch=1,
            grid=(cols // step,),
            in_specs=[col] * (2 * pieces) + [whole] * 3,
            out_specs=[out, out, pl.BlockSpec((units, pieces * cols), lambda i, s: (0, 0))],
        ),
        out_shape=[jax.ShapeDtypeStruct((pieces, cols, units), F32)] * 2
        + [jax.ShapeDtypeStruct((units, pieces * cols), F32)],
        cost_estimate=flops(6 * slots * cols * units * pieces),
    )(place, *ins, *ups, gate_term, up_term, product)
    width = pieces * cols
    return gate_grad.reshape(width, units), up_grad.reshape(width, units), down_grad


def expert_body(place_ref, *refs):
    ups, downs = refs[0:2], refs[2:4]
    partial_ref, gate_pre_ref, up_pre_ref = refs[4:7]
    outs = (len(refs) - 10) // 3
    gates, upws = refs[7 : 7 + outs], refs[7 + outs : 7 + 2 * outs]
    product_ref, gate_term_ref, up_term_ref = refs[7 + 2 * outs : 10 + 2 * outs]
    rows = refs[10 + 2 * outs :]
    unit_grad = partial_ref[...]
    for x, w in zip(ups, downs):
        unit_grad = unit_grad + dot(x[...], w[...], COLS)
    gate_pre = gate_pre_ref[...]
    up_pre = up_pre_ref[...]
    sigma = jax.nn.sigmoid(gate_pre)
    active = gate_pre * sigma
    product_ref[...] = (active * up_pre).astype(BF16)
    gate_term = (unit_grad * up_pre * sigma * (1.0 + gate_pre * (1.0 - sigma))).astype(BF16)
    up_term = (unit_grad * active).astype(BF16)
    gate_term_ref[...] = gate_term
    up_term_ref[...] = up_term
    for g, u, out in zip(gates, upws, rows):
        out[...] = (dot(gate_term, g[...], COLS) + dot(up_term, u[...], COLS)).astype(BF16)


def expert_call(place, ups, partial, gate_pre, up_pre, down, gate, up):
    slots, cols = ups[0].shape
    units = gate.shape[1]
    pieces = gate.shape[0] // cols
    step = math.gcd(slots, 256)
    row = lambda width: pl.BlockSpec((step, width), lambda i, s: (i, 0))
    down_of = lambda k: pl.BlockSpec((units, cols), lambda i, s, k=k: (0, s[0] ^ k))
    weight_of = lambda k: pl.BlockSpec((cols, units), lambda i, s, k=k: (s[0] ^ k, 0))
    weights = [weight_of(k) for k in range(pieces)]
    return pl.pallas_call(
        expert_body,
        grid_spec=pltpu.PrefetchScalarGridSpec(
            num_scalar_prefetch=1,
            grid=(slots // step,),
            in_specs=[row(cols)] * 2
            + [down_of(pieces - 2), down_of(pieces - 1)]
            + [row(units)] * 3
            + weights
            + weights,
            out_specs=[row(units)] * 3 + [row(cols)] * pieces,
        ),
        out_shape=[jax.ShapeDtypeStruct((slots, units), BF16)] * 3
        + [jax.ShapeDtypeStruct((slots, cols), BF16)] * pieces,
        cost_estimate=flops(6 * slots * cols * units * pieces),
    )(place, *ups, down, down, partial, gate_pre, up_pre, *[gate] * pieces, *[up] * pieces)


def proj_body(ids_ref, *refs):
    pieces, (even_ref, odd_ref, out_ref, rows_ref) = refs[:-4], refs[-4:]
    count, rows, _ = pieces[0].shape
    for k, piece in enumerate(pieces):
        start = pl.multiple_of((ids_ref[0] ^ k) * rows, rows)
        for source in range(count):
            rows_ref[source, pl.ds(start, rows), :] = piece[source]
    total = None
    for k in range(count):
        kept_ref = odd_ref if k % 2 else even_ref
        part = dot(rows_ref[ids_ref[1] ^ k], kept_ref[k // 2], ROWS)
        total = part if total is None else total + part
    out_ref[...] = total


def dot(a, b, dims=None):
    if dims is None:
        return jnp.dot(a, b, preferred_element_type=F32)
    return lax.dot_general(a, b, dims, preferred_element_type=F32)


def carry_pair(state, span, reverse):
    low = lax.axis_index("sp") % 2
    first = (low == 1) if reverse else (low == 0)
    mine, sent = state
    theirs = swap(sent, "sp", 1).astype(F32)
    mine = mine.astype(F32)
    early = jnp.where(first, mine, theirs)
    late = jnp.where(first, theirs, mine)
    return early, (late + jnp.exp(span) * early).astype(BF16)


def carry_outer(total, reverse):
    count = lax.axis_size("sp")
    sign = -2 if reverse else 2
    return [
        lax.ppermute(
            total, "sp", [(i, i + sign * d) for i in range(count) if 0 <= i + sign * d < count]
        )
        for d in range(1, count // 2)
    ]


def carry_inner(early, outer, span, reverse):
    low = lax.axis_index("sp") % 2
    first = (low == 1) if reverse else (low == 0)
    ahead = jnp.zeros(early.shape, F32)
    for d, piece in enumerate(outer, 1):
        ahead = ahead + jnp.exp(span * (2 * d - 2)) * piece.astype(F32)
    behind = early + jnp.exp(span) * ahead
    own = jnp.where(first, ahead, behind).astype(BF16)
    return own, jnp.where(first, behind, ahead).astype(BF16)


def local(
    hidden,
    cotangent,
    retained,
    queries,
    key_rows,
    value_rows,
    routes,
    route_weight,
    gate_weight,
    up_weight,
    down_weight,
    out_weight,
):
    sp_count = lax.axis_size("sp")
    tp_count = lax.axis_size("tp")
    sp_place = lax.axis_index("sp")
    tp_place = lax.axis_index("tp")
    tokens, width = hidden.shape
    ids = jnp.stack([tp_place, sp_place])
    rates = jnp.stack(head_rates(tp_place, tokens * sp_count))
    log_gamma = rates[0]
    top = routes.shape[1]
    capacity = 3 * tokens * top // (2 * sp_count)
    slots = sp_count * capacity
    col_width = width // tp_count
    gate, up, down = gate_weight[0], up_weight[0], down_weight[0]

    flat = routes.T.reshape(-1)
    order = jnp.arange(flat.shape[0], dtype=jnp.int32)
    before = (flat[None, :] == flat[:, None]) & (order[None, :] < order[:, None])
    rank = jnp.sum(before.astype(jnp.int32), axis=1)
    target = ((flat ^ sp_place) * capacity + rank).reshape(top, tokens)
    place_of = jnp.arange(slots, dtype=jnp.int32)[:, None]
    picks = [(place_of == target[r][None, :]).astype(BF16) for r in range(top)]
    pick_all = sum(picks[1:], picks[0])
    hid_cols = lax.dynamic_slice_in_dim(hidden, tp_place * col_width, col_width, 1)
    cot_cols = lax.dynamic_slice_in_dim(cotangent, tp_place * col_width, col_width, 1)
    cot_wide = cot_cols.astype(F32)
    upstream = jnp.concatenate(
        [(route_weight[:, r : r + 1] * cot_wide).astype(BF16) for r in range(top)], axis=0
    )
    in_send = dot(pick_all, hid_cols).astype(BF16).reshape(sp_count, capacity, col_width)
    up_send = (
        dot(jnp.concatenate(picks, axis=1), upstream)
        .astype(BF16)
        .reshape(sp_count, capacity, col_width)
    )
    got_in = join(in_send, exchange(in_send)).reshape(slots, col_width)
    got_up = join(up_send, exchange(up_send)).reshape(slots, col_width)
    place = jnp.arange(tokens, dtype=F32)
    span = log_gamma * tokens
    suffix_decay = jnp.exp(log_gamma * (tokens - place))[:, None]
    prefix_decay = jnp.exp(log_gamma * (place + 1.0))[:, None]
    key_decayed = (key_rows.astype(F32) * suffix_decay).astype(BF16)
    query_decayed = (queries.astype(F32) * prefix_decay).astype(BF16)
    prior_state = dot(key_decayed, value_rows, ROWS).astype(BF16)
    state_rows = prior_state.shape[0] // 2
    low = sp_place % 2
    halves = [
        lax.dynamic_slice_in_dim(prior_state, place * state_rows, state_rows, 0)
        for place in (low, 1 - low)
    ]
    prior_early, prior_total = carry_pair(halves, span, False)
    ins = gather_tp(got_in)
    ups = gather_tp(got_up)
    kept = [retained] + [swap(retained, "sp", k) for k in range(2, sp_count, 2)]
    prior_outer = carry_outer(prior_total, False)
    blocks = [tp_place ^ k for k in range(tp_count)]
    downs = [lax.dynamic_slice_in_dim(down, b * col_width, col_width, 1) for b in blocks[:-2]]
    gate_pre, up_pre = pre_call(ids, ins, gate, up)
    partial = sum(dot(x, w, COLS) for x, w in zip(ups, downs))
    product, gate_term, up_term, *row_parts = expert_call(
        ids, ups[-2:], partial, gate_pre, up_pre, down, gate, up
    )
    row_grad = scatter_tp(row_parts).astype(BF16)
    row_grad = row_grad.reshape(sp_count, capacity, col_width)
    returned = exchange(row_grad)
    even = jnp.stack(kept)
    odd = swap(even, "sp", 1)
    prior_own, prior_sent = carry_inner(prior_early, prior_outer, span, False)
    prior_got = swap(prior_sent, "sp", 1)
    (layer_cols,) = call(
        layer_body,
        (((tokens, col_width), BF16),),
        pick_all.reshape(sp_count, capacity, tokens),
        row_grad,
        *returned,
        cot_cols,
        work=2 * slots * tokens * col_width,
    )

    gate_grad, up_grad, down_grad = grad_call(
        ids, ins, ups, gate_term, up_term, product
    )

    layers = gather_tp(layer_cols)
    values = value_rows.shape[1]
    part = width // sp_count
    layer_send, mixed_grad, *state = call(
        mix_body,
        (
            ((sp_count, tokens // tp_count, part), BF16),
            ((tokens, values), BF16),
            ((queries.shape[1] // 2, values), BF16),
            ((queries.shape[1] // 2, values), BF16),
        ),
        *layers,
        out_weight,
        query_decayed,
        scalars=(ids,),
        work=2 * tokens * width * values,
    )

    later_early, later_total = carry_pair(state, span, True)
    later_outer = carry_outer(later_total, True)
    mine = transpose_blocks(layer_send)
    later_own, later_sent = carry_inner(later_early, later_outer, span, True)
    later_got = swap(later_sent, "sp", 1)
    layer_rows = gather_tp(mine)
    query_gradient, key_near, value_near = call(
        near_body,
        ((queries.shape, F32), (queries.shape, F32), (value_rows.shape, F32)),
        mixed_grad,
        queries,
        key_rows,
        value_rows,
        prior_own,
        prior_got,
        scalars=(ids, rates),
        work=10 * tokens * tokens * values,
    )
    key_gradient, value_gradient, proj_grad = call(
        last_body,
        ((key_near.shape, F32), (value_near.shape, F32), ((part, retained.shape[1]), F32)),
        later_own,
        later_got,
        key_rows,
        value_rows,
        key_near,
        value_near,
        *layer_rows,
        even,
        odd,
        scalars=(ids, rates),
        work=2 * sp_count * tokens * part * retained.shape[1],
        scratch=(((sp_count, tokens, part), BF16),),
    )
    return (
        gate_grad[None],
        up_grad[None],
        down_grad[None],
        proj_grad,
        query_gradient,
        key_gradient,
        value_gradient,
    )


def solution(mesh):
    return jax.shard_map(
        local,
        mesh=mesh,
        in_specs=(
            P("sp", None),
            P("sp", None),
            P("sp", "tp"),
            P("sp", "tp"),
            P("sp", "tp"),
            P("sp", "tp"),
            P("sp", None),
            P("sp", None),
            P("sp", None, "tp"),
            P("sp", None, "tp"),
            P("sp", "tp", None),
            P(None, "tp"),
        ),
        out_specs=(
            P("sp", None, "tp"),
            P("sp", None, "tp"),
            P("sp", "tp", None),
            P("sp", "tp"),
            P("sp", "tp"),
            P("sp", "tp"),
            P("sp", "tp"),
        ),
        check_vma=False,
    )
```
